32 devices in a mesh: fs: 8 (over z, core), tp: 4 (over y, x).
Axes of the slice: x: 2, y: 2, z: 4, core: 2. Of those that a mesh axis runs over, the one named last changes fastest.
Arguments:
- tokens: bfloat16 [4096, 4096], P('fs', 'tp'), may hold values from -16 to 16
- norm_gain: float32 [4096], P('fs'), may hold values from 0.1 to 1.9
- gate_train: float32 [4096, 12288], P('fs', 'tp'), may hold values from -6 to 6
- up_train: float32 [4096, 12288], P('fs', 'tp'), may hold values from -6 to 6
Outputs:
- gate_serve: bfloat16 [4096, 12288], P(None, 'tp')
- up_serve: bfloat16 [4096, 12288], P(None, 'tp')
- hidden: bfloat16 [4096, 12288], P('fs', 'tp')
The draws below stay inside these ranges and needn't reach their ends.
All inputs are finite; a program needn't handle non-finite values.
Results may differ from the reference program's by a relative error of at most 0.0071.
Values may be sent and summed in bfloat16 or wider, within the bound.
A program may use at most 192 MiB of HBM per device.

```python
import jax
import jax.numpy as jnp
from jax import lax

D = 4096
FF = 12288
TOKENS = 4096


def steps_of(rng, extent, split, low, largest):
    loudness, own = 1.0, jax.random.fold_in(rng, 6)
    for position, parts in split:
        heights = jnp.exp(jax.random.uniform(jax.random.fold_in(own, position), (parts,), jnp.float32, low / len(split), largest / len(split)))
        loudness = loudness * jnp.repeat(heights, extent[position] // parts).reshape([-1 if axis == position else 1 for axis in range(len(extent))])
    return loudness


def scatter_about(key, dims, width, reach, cuts=(), held_as=jnp.bfloat16):
    values = jax.random.normal(key, dims, jnp.float32) * width
    if len(cuts) > 0:
        values = steps_of(key, dims, cuts, -0.22, 0.18) * values
    return jnp.clip(values, min=-reach, max=reach).astype(held_as)


def setup_inputs(seed: int = 0) -> dict:
    keys = jax.random.split(jax.random.key(seed), 5)
    tokens = scatter_about(keys[0], (TOKENS, D), 3.0, 16.0, ((0, 8), (1, 4)))
    norm_gain = jnp.clip(1.0 + 0.18 * jax.random.normal(keys[1], (D,), jnp.float32), 0.1, 1.9)
    gate_train = scatter_about(keys[2], (D, FF), 1.0, 6.0, ((0, 8), (1, 4)), jnp.float32)
    up_train = scatter_about(keys[3], (D, FF), 1.0, 6.0, ((0, 8), (1, 4)), jnp.float32)
    return dict(tokens=tokens, norm_gain=norm_gain, gate_train=gate_train, up_train=up_train)


def reference(tokens, norm_gain, gate_train, up_train):
    gain = norm_gain.astype(jnp.float32)[:, None]
    gate_serve = (gate_train * gain).astype(jnp.bfloat16)
    up_serve = (up_train * gain).astype(jnp.bfloat16)
    values = tokens.astype(jnp.float32)
    normed = (values * jax.lax.rsqrt(lax.optimization_barrier(jnp.mean(values * values, axis=-1, keepdims=True)) + 1e-06)).astype(jnp.bfloat16)
    scale = D ** (-0.5)
    gate = jnp.dot(normed, gate_serve, preferred_element_type=jnp.float32) * scale
    up = jnp.dot(normed, up_serve, preferred_element_type=jnp.float32) * scale
    hidden = (jax.nn.silu(gate) * up).astype(jnp.bfloat16)
    return (gate_serve, up_serve, hidden)
```

```python
import functools

import jax
import jax.numpy as jnp
from jax import lax
from jax.experimental import pallas as pl
from jax.experimental.pallas import tpu as pltpu
from jax.sharding import PartitionSpec as P

PIECES = 3


def product(normed_ref, weight_ref, scale):
    return jnp.dot(normed_ref[...], weight_ref[...], preferred_element_type=jnp.float32) * scale


def gate_kernel(scale, normed_ref, weight_ref, *refs):
    serve_ref, gate_ref = refs[-2:]
    serve_ref[...] = weight_ref[...]
    gate_ref[...] = product(normed_ref, weight_ref, scale)


def up_kernel(scale, normed_ref, weight_ref, gate_ref, *refs):
    serve_ref, hidden_ref = refs[-2:]
    serve_ref[...] = weight_ref[...]
    gate = gate_ref[...]
    up = product(normed_ref, weight_ref, scale)
    hidden_ref[...] = (gate / (1.0 + jnp.exp(-gate)) * up).astype(hidden_ref.dtype)


def step(kernel, scale, at, cols, normed, weight, gate, kept):
    depth, width = weight.shape
    toks = normed.shape[0]
    tile = 256 if width % 256 == 0 else width
    first = at * (width // tile)
    here = pl.BlockSpec((depth, tile), lambda i: (0, first + i))
    piece = pl.BlockSpec((depth, tile), lambda i: (0, i))
    local = pl.BlockSpec((toks, tile), lambda i: (0, i))
    there = pl.BlockSpec((toks, tile), lambda i: (0, first + i))
    args, specs = [normed, weight], [pl.BlockSpec((toks, depth), lambda i: (0, 0)), piece]
    serve = jax.ShapeDtypeStruct((depth, cols), weight.dtype)
    if gate is None:
        outs, out_specs = [serve, jax.ShapeDtypeStruct((toks, width), jnp.float32)], [here, local]
    else:
        args.append(gate)
        specs.append(local)
        outs, out_specs = [serve, jax.ShapeDtypeStruct((toks, cols), weight.dtype)], [here, there]
    aliases = {len(args) + k: k for k in range(len(kept))}
    return pl.pallas_call(
        functools.partial(kernel, scale),
        grid=(width // tile,),
        in_specs=specs + [pl.BlockSpec(memory_space=pl.ANY)] * len(kept),
        out_specs=out_specs,
        out_shape=outs,
        input_output_aliases=aliases,
        cost_estimate=pl.CostEstimate(
            flops=2 * toks * depth * width, bytes_accessed=4 * depth * width + 2 * toks * depth, transcendentals=0
        ),
        compiler_params=pltpu.CompilerParams(vmem_limit_bytes=40 * 1024 * 1024),
    )(*args, *kept)


def body(tokens, norm_gain, gate_train, up_train):
    gain = norm_gain[:, None]
    cols = gate_train.shape[1]
    width = cols // PIECES

    def gathered(train, at):
        local = (train[:, at * width : (at + 1) * width] * gain).astype(jnp.bfloat16)
        return lax.all_gather(local, "fs", axis=0, tiled=True)

    tp, mine = lax.axis_size("tp"), lax.axis_index("tp")
    toks, part = tokens.shape
    whole = jnp.zeros((toks, tp * part), tokens.dtype)
    for k in range(tp):
        got = tokens if k == 0 else lax.ppermute(tokens, "tp", [(i, (i + k) % tp) for i in range(tp)])
        whole = lax.dynamic_update_slice(whole, got, (0, lax.rem(mine + tp - k, tp) * part))
    values = whole.astype(jnp.float32)
    normed = (values * lax.rsqrt(jnp.mean(values * values, axis=-1, keepdims=True) + 1e-06)).astype(jnp.bfloat16)
    scale = normed.shape[1] ** (-0.5)

    gates = [gathered(gate_train, at) for at in range(PIECES)]
    ups = [gathered(up_train, at) for at in range(PIECES)]
    gate_kept, up_kept, gate = [], [], []
    for at in range(PIECES):
        served, value = step(gate_kernel, scale, at, cols, normed, gates[at], None, gate_kept)
        gate_kept = [served]
        gate.append(value)
    for at in range(PIECES):
        up_kept = step(up_kernel, scale, at, cols, normed, ups[at], gate[at], up_kept)
    return (gate_kept[0], *up_kept)


def solution(mesh):
    in_specs = (P("fs", "tp"), P("fs"), P("fs", "tp"), P("fs", "tp"))
    out_specs = (P(None, "tp"), P(None, "tp"), P("fs", "tp"))
    return jax.shard_map(body, mesh=mesh, in_specs=in_specs, out_specs=out_specs, check_vma=False)
```

```python
import functools

import jax
import jax.numpy as jnp
from jax import lax
from jax.experimental import pallas as pl
from jax.experimental.pallas import tpu as pltpu
from jax.sharding import PartitionSpec as P

VMEM = 56 * 1024 * 1024


def call(kernel, grid, in_specs, out_specs, out_shape, flops, moved, aliases=None):
    return pl.pallas_call(
        kernel,
        grid=(grid,),
        in_specs=in_specs,
        out_specs=out_specs,
        out_shape=out_shape,
        input_output_aliases=aliases or {},
        cost_estimate=pl.CostEstimate(flops=flops, bytes_accessed=moved, transcendentals=0),
        compiler_params=pltpu.CompilerParams(vmem_limit_bytes=VMEM),
    )


def fold_kernel(gates, gain_ref, gate_ref, up_ref, out_ref):
    @pl.when(pl.program_id(0) < gates)
    def _():
        out_ref[...] = (gate_ref[...] * gain_ref[...]).astype(out_ref.dtype)

    @pl.when(pl.program_id(0) >= gates)
    def _():
        out_ref[...] = (up_ref[...] * gain_ref[...]).astype(out_ref.dtype)


def product(normed_ref, weight_ref, scale):
    return jnp.dot(normed_ref[...], weight_ref[...], preferred_element_type=jnp.float32) * scale


def gated(gate, up):
    return gate / (1.0 + jnp.exp(-gate)) * up


def both_kernel(scale, normed_ref, gate_ref, up_ref, gate_out, up_out, hidden_ref):
    gate_out[...] = gate_ref[...]
    up_out[...] = up_ref[...]
    gate = product(normed_ref, gate_ref, scale)
    hidden_ref[...] = gated(gate, product(normed_ref, up_ref, scale)).astype(hidden_ref.dtype)


def gate_kernel(scale, normed_ref, weight_ref, _, serve_ref, gate_ref):
    serve_ref[...] = weight_ref[...]
    gate_ref[...] = product(normed_ref, weight_ref, scale)


def up_kernel(scale, normed_ref, weight_ref, gate_ref, _, __, serve_ref, hidden_ref):
    serve_ref[...] = weight_ref[...]
    hidden_ref[...] = gated(gate_ref[...], product(normed_ref, weight_ref, scale)).astype(hidden_ref.dtype)


def body(tokens, norm_gain, gate_train, up_train):
    gain = norm_gain[:, None]
    rows, cols = gate_train.shape
    last = max(cols // 4 // 128, 1) * 128
    while cols % last:
        last -= 128
    first = cols - last

    gates, tiles = cols // last, (cols + first) // last
    block = lambda index: pl.BlockSpec((rows, last), index)
    local = call(
        functools.partial(fold_kernel, gates),
        tiles,
        [
            pl.BlockSpec((rows, 1), lambda i: (0, 0)),
            block(lambda i: (0, jnp.minimum(i, gates - 1))),
            block(lambda i: (0, jnp.maximum(i - gates, 0))),
        ],
        block(lambda i: (0, i)),
        jax.ShapeDtypeStruct((rows, cols + first), jnp.bfloat16),
        2 * rows * (cols + first),
        6 * rows * (cols + first),
    )(gain, gate_train, up_train)
    main = lax.all_gather(local, "fs", axis=0, tiled=True)
    rest = lax.all_gather((up_train[:, first:] * gain).astype(jnp.bfloat16), "fs", axis=0, tiled=True)

    tp, mine = lax.axis_size("tp"), lax.axis_index("tp")
    toks, part = tokens.shape
    whole = jnp.zeros((toks, tp * part), tokens.dtype)
    for k in range(tp):
        got = tokens if k == 0 else lax.ppermute(tokens, "tp", [(i, (i + k) % tp) for i in range(tp)])
        whole = lax.dynamic_update_slice(whole, got, (0, lax.rem(mine + tp - k, tp) * part))
    values = whole.astype(jnp.float32)
    normed = (values * lax.rsqrt(jnp.mean(values * values, axis=-1, keepdims=True) + 1e-06)).astype(jnp.bfloat16)
    depth = normed.shape[1]
    scale = depth ** (-0.5)

    tile = 256 if last % 256 == 0 else 128
    n_all, n_first, n_last = cols // tile, first // tile, last // tile
    resident = pl.BlockSpec((toks, depth), lambda i: (0, 0))
    weight = lambda at: pl.BlockSpec((depth, tile), lambda i: (0, at + i))
    units = lambda at: pl.BlockSpec((toks, tile), lambda i: (0, at + i))
    anywhere = pl.BlockSpec(memory_space=pl.ANY)
    serve = jax.ShapeDtypeStruct((depth, cols), jnp.bfloat16)
    hidden = jax.ShapeDtypeStruct((toks, cols), jnp.bfloat16)
    flops, moved = 2 * toks * depth * tile, 4 * depth * tile

    gate_serve, up_serve, out = call(
        functools.partial(both_kernel, scale),
        n_first,
        [resident, weight(0), weight(n_all)],
        [weight(0), weight(0), units(0)],
        [serve, serve, hidden],
        2 * n_first * flops,
        2 * n_first * moved,
    )(normed, main, main)
    gate_serve, gate = call(
        functools.partial(gate_kernel, scale),
        n_last,
        [resident, weight(n_first), anywhere],
        [weight(n_first), units(0)],
        [serve, jax.ShapeDtypeStruct((toks, last), jnp.float32)],
        n_last * flops,
        n_last * moved,
        {2: 0},
    )(normed, main, gate_serve)
    up_serve, out = call(
        functools.partial(up_kernel, scale),
        n_last,
        [resident, weight(0), units(0), anywhere, anywhere],
        [weight(n_first), units(n_first)],
        [serve, hidden],
        n_last * flops,
        n_last * moved,
        {3: 0, 4: 1},
    )(normed, rest, gate, up_serve, out)
    return gate_serve, up_serve, out


def solution(mesh):
    in_specs = (P("fs", "tp"), P("fs"), P("fs", "tp"), P("fs", "tp"))
    out_specs = (P(None, "tp"), P(None, "tp"), P("fs", "tp"))
    return jax.shard_map(body, mesh=mesh, in_specs=in_specs, out_specs=out_specs, check_vma=False)
```

```python
import functools

import jax
import jax.numpy as jnp
from jax import lax
from jax.experimental import pallas as pl
from jax.experimental.pallas import tpu as pltpu
from jax.sharding import PartitionSpec as P

VMEM = 56 * 1024 * 1024
CORES = 2
PIECES = 4


def call(kernel, grid, in_specs, out_specs, out_shape, flops, moved, aliases=None):
    return pl.pallas_call(
        kernel,
        grid=(grid,),
        in_specs=in_specs,
        out_specs=out_specs,
        out_shape=out_shape,
        input_output_aliases=aliases or {},
        cost_estimate=pl.CostEstimate(flops=flops, bytes_accessed=moved, transcendentals=0),
        compiler_params=pltpu.CompilerParams(vmem_limit_bytes=VMEM),
    )


def fold_kernel(gates, gain_ref, gate_ref, up_ref, out_ref):
    @pl.when(pl.program_id(0) < gates)
    def _():
        out_ref[...] = (gate_ref[...] * gain_ref[...]).astype(out_ref.dtype)

    @pl.when(pl.program_id(0) >= gates)
    def _():
        out_ref[...] = (up_ref[...] * gain_ref[...]).astype(out_ref.dtype)


def line_kernel(chips, tp, local_ref, tok_ref, out_ref, all_ref, own_sem, tok_send, tok_recv, send, recv, pass_send, pass_recv):
    me = lax.axis_index("fs")
    z, core = me // CORES, me % CORES
    piece = local_ref.shape[0] // PIECES
    up, down = lax.rem(z + 1, chips), lax.rem(z + chips - 1, chips)
    peer = z * CORES + (1 - core)

    barrier = pltpu.get_barrier_semaphore()
    for device in (up * CORES + core, down * CORES + core, peer):
        pl.semaphore_signal(barrier, inc=1, device_id={"fs": device}, device_id_type=pl.DeviceIdType.MESH)
    mine = lax.axis_index("tp")
    for k in range(1, tp):
        pl.semaphore_signal(
            barrier, inc=1, device_id={"tp": lax.rem(mine + k, tp)}, device_id_type=pl.DeviceIdType.MESH
        )
    pl.semaphore_wait(barrier, 3 + tp - 1)

    part = tok_ref.shape[1]

    def features(k):
        return pltpu.make_async_remote_copy(
            src_ref=tok_ref, dst_ref=all_ref.at[:, pl.ds(pl.multiple_of(mine * part, 128), part)],
            send_sem=tok_send.at[k], recv_sem=tok_recv.at[k],
            device_id={"tp": lax.rem(mine + k, tp)}, device_id_type=pl.DeviceIdType.MESH,
        )

    def rows(q):
        return pl.ds(q * piece, piece)

    def move(src, block, q, device, send_sem, recv_sem):
        return pltpu.make_async_remote_copy(
            src_ref=src, dst_ref=out_ref.at[block, rows(q)], send_sem=send_sem, recv_sem=recv_sem,
            device_id={"fs": device}, device_id_type=pl.DeviceIdType.MESH,
        )

    def held(way, p):
        chip = z - p if way == 0 else z + p
        there = chip >= 0 if way == 0 else chip < chips
        return lax.clamp(0, chip, chips - 1), there

    def hop(way, p, q, src):
        chip, there = held(way, p)
        onward = there & (z < chips - 1 if way == 0 else z > 0)
        block = chip * CORES + core
        src = out_ref.at[block, rows(q)] if src is None else src
        device = (up if way == 0 else down) * CORES + core
        return onward, move(src, block, q, device, send.at[way, p, q], recv.at[way, p, q])

    def arrival(way, p, q):
        chip, there = held(way, p + 1)
        here = out_ref.at[chip * CORES + core, rows(q)]
        return there, move(here, chip * CORES + core, q, peer, send.at[way, p, q], recv.at[way, p, q])

    def passing(way, p, q, src, mine):
        chip, there = held(way, p)
        block = chip * CORES + (core if mine else 1 - core)
        src = out_ref.at[block, rows(q)] if src is None else src
        return there, move(src, block, q, peer, pass_send.at[way, p, q], pass_recv.at[way, p, q])

    own = pltpu.make_async_copy(local_ref, out_ref.at[me], own_sem)
    for q in range(PIECES):
        for way in range(2):
            onward, copy = hop(way, 0, q, local_ref.at[rows(q)])
            pl.when(onward)(copy.start)
    for q in range(PIECES):
        passing(0, 0, q, local_ref.at[rows(q)], True)[1].start()
    own.start()
    for k in range(1, tp):
        features(k).start()
    own_features = pltpu.make_async_copy(
        tok_ref, all_ref.at[:, pl.ds(pl.multiple_of(mine * part, 128), part)], tok_send.at[0]
    )
    own_features.start()

    @pl.loop(1, chips)
    def _(p):
        for q in range(PIECES):
            for way in range(2):
                there, copy = arrival(way, p - 1, q)
                pl.when(there)(copy.wait_recv)
                onward, copy = hop(way, p, q, None)
                pl.when(onward)(copy.start)
                there, copy = passing(way, p, q, None, True)
                pl.when(there)(copy.start)

    own.wait()
    own_features.wait()
    for k in range(1, tp):
        features(k).wait()
    for q in range(PIECES):
        copy = passing(0, 0, q, local_ref.at[rows(q)], True)[1]
        copy.wait_send()
        passing(0, 0, q, None, False)[1].wait_recv()
        for way in range(2):
            onward, copy = hop(way, 0, q, local_ref.at[rows(q)])
            pl.when(onward)(copy.wait_send)

    @pl.loop(1, chips)
    def _(p):
        for q in range(PIECES):
            for way in range(2):
                onward, copy = hop(way, p, q, None)
                pl.when(onward)(copy.wait_send)
                there, copy = passing(way, p, q, None, True)
                pl.when(there)(copy.wait_send)
                there, copy = passing(way, p, q, None, False)
                pl.when(there)(copy.wait_recv)


def line_gather(local, tokens):
    tp = lax.axis_size("tp")
    toks, part = tokens.shape
    fs = lax.axis_size("fs")
    chips = fs // CORES
    (rows, width) = local.shape
    sems = pltpu.SemaphoreType.DMA((2, chips, PIECES))
    tok_sems = pltpu.SemaphoreType.DMA((tp,))
    out, whole = pl.pallas_call(
        functools.partial(line_kernel, chips, tp),
        in_specs=[pl.BlockSpec(memory_space=pl.ANY)] * 2,
        out_specs=[pl.BlockSpec(memory_space=pl.ANY)] * 2,
        out_shape=[
            jax.ShapeDtypeStruct((fs, rows, width), local.dtype),
            jax.ShapeDtypeStruct((toks, tp * part), tokens.dtype),
        ],
        scratch_shapes=[pltpu.SemaphoreType.DMA, tok_sems, tok_sems, sems, sems, sems, sems],
        cost_estimate=pl.CostEstimate(flops=2 * 10**11, bytes_accessed=2 * fs * rows * width, transcendentals=0),
        compiler_params=pltpu.CompilerParams(collective_id=0, has_side_effects=True, vmem_limit_bytes=VMEM),
    )(local, tokens)
    return out.reshape(fs * rows, width), whole


def product(normed_ref, weight_ref, scale):
    return jnp.dot(normed_ref[...], weight_ref[...], preferred_element_type=jnp.float32) * scale


def gated(gate, up):
    return gate / (1.0 + jnp.exp(-gate)) * up


def both_kernel(scale, normed_ref, gate_ref, up_ref, gate_out, up_out, hidden_ref):
    gate_out[...] = gate_ref[...]
    up_out[...] = up_ref[...]
    gate = product(normed_ref, gate_ref, scale)
    hidden_ref[...] = gated(gate, product(normed_ref, up_ref, scale)).astype(hidden_ref.dtype)


def gate_kernel(scale, normed_ref, weight_ref, _, serve_ref, gate_ref):
    serve_ref[...] = weight_ref[...]
    gate_ref[...] = product(normed_ref, weight_ref, scale)


def up_kernel(scale, normed_ref, weight_ref, gate_ref, _, __, serve_ref, hidden_ref):
    serve_ref[...] = weight_ref[...]
    hidden_ref[...] = gated(gate_ref[...], product(normed_ref, weight_ref, scale)).astype(hidden_ref.dtype)


def body(tokens, norm_gain, gate_train, up_train):
    gain = norm_gain[:, None]
    rows, cols = gate_train.shape
    last = max(cols // 4 // 128, 1) * 128
    while cols % last:
        last -= 128
    first = cols - last

    gates, tiles = cols // last, (cols + first) // last
    block = lambda index: pl.BlockSpec((rows, last), index)
    local = call(
        functools.partial(fold_kernel, gates),
        tiles,
        [
            pl.BlockSpec((rows, 1), lambda i: (0, 0)),
            block(lambda i: (0, jnp.minimum(i, gates - 1))),
            block(lambda i: (0, jnp.maximum(i - gates, 0))),
        ],
        block(lambda i: (0, i)),
        jax.ShapeDtypeStruct((rows, cols + first), jnp.bfloat16),
        2 * rows * (cols + first),
        6 * rows * (cols + first),
    )(gain, gate_train, up_train)
    (main, whole), rest = lax.optimization_barrier(
        (line_gather(local, tokens), (up_train[:, first:] * gain).astype(jnp.bfloat16))
    )
    rest = lax.all_gather(rest, "fs", axis=0, tiled=True)
    toks = tokens.shape[0]
    values = whole.astype(jnp.float32)
    normed = (values * lax.rsqrt(jnp.mean(values * values, axis=-1, keepdims=True) + 1e-06)).astype(jnp.bfloat16)
    depth = normed.shape[1]
    scale = depth ** (-0.5)

    tile = 256 if last % 256 == 0 else 128
    n_all, n_first, n_last = cols // tile, first // tile, last // tile
    resident = pl.BlockSpec((toks, depth), lambda i: (0, 0))
    weight = lambda at: pl.BlockSpec((depth, tile), lambda i: (0, at + i))
    units = lambda at: pl.BlockSpec((toks, tile), lambda i: (0, at + i))
    anywhere = pl.BlockSpec(memory_space=pl.ANY)
    serve = jax.ShapeDtypeStruct((depth, cols), jnp.bfloat16)
    hidden = jax.ShapeDtypeStruct((toks, cols), jnp.bfloat16)
    flops, moved = 2 * toks * depth * tile, 4 * depth * tile

    gate_serve, up_serve, out = call(
        functools.partial(both_kernel, scale),
        n_first,
        [resident, weight(0), weight(n_all)],
        [weight(0), weight(0), units(0)],
        [serve, serve, hidden],
        2 * n_first * flops,
        2 * n_first * moved,
    )(normed, main, main)
    gate_serve, gate = call(
        functools.partial(gate_kernel, scale),
        n_last,
        [resident, weight(n_first), anywhere],
        [weight(n_first), units(0)],
        [serve, jax.ShapeDtypeStruct((toks, last), jnp.float32)],
        n_last * flops,
        n_last * moved,
        {2: 0},
    )(normed, main, gate_serve)
    up_serve, out = call(
        functools.partial(up_kernel, scale),
        n_last,
        [resident, weight(0), units(0), anywhere, anywhere],
        [weight(n_first), units(n_first)],
        [serve, hidden],
        n_last * flops,
        n_last * moved,
        {3: 0, 4: 1},
    )(normed, rest, gate, up_serve, out)
    return gate_serve, up_serve, out


def solution(mesh):
    in_specs = (P("fs", "tp"), P("fs"), P("fs", "tp"), P("fs", "tp"))
    out_specs = (P(None, "tp"), P(None, "tp"), P("fs", "tp"))
    return jax.shard_map(body, mesh=mesh, in_specs=in_specs, out_specs=out_specs, check_vma=False)
```
